256 devices in a mesh: sp: 64 (over z, y, core), tp: 4 (over x).
Axes of the slice: x: 4, y: 4, z: 8, core: 2. Of those that a mesh axis runs over, the one named last changes fastest.
Arguments:
- gate_in: bfloat16 [32768, 2048], P('sp', 'tp'), may hold values from -6 to 6
- value_in: bfloat16 [32768, 2048], P('sp', 'tp'), may hold values from -6 to 6
- gate_out: bfloat16 [32768, 2048], P('sp', 'tp'), may hold values from -6 to 6
- conv_taps: float32 [3, 2048], P(None, 'tp'), may hold values from -3.5 to 3.5
- proj_weight: bfloat16 [2048, 2048], P('tp'), may hold values from -0.125 to 0.125
- residual: bfloat16 [32768, 2048], P(('sp', 'tp')), may hold values from -6 to 6
- norm_gain: float32 [2048], replicated, may hold values from 0.1 to 1.9
- routes: int32 [32768, 2], P('sp'), may hold values from 0 to 63, all different within a row; in each aligned block of 128 rows (0 to 127, 128 to 255, ...) at most 8 rows name the same one
- route_weight: float32 [32768, 2], P('sp'), may hold values from 0.1 to 0.9
- expert_gate: bfloat16 [64, 2048, 2048], P('sp', None, 'tp'), may hold values from -0.125 to 0.125
- expert_up: bfloat16 [64, 2048, 2048], P('sp', None, 'tp'), may hold values from -0.125 to 0.125
- expert_down: bfloat16 [64, 2048, 2048], P('sp', 'tp'), may hold values from -0.125 to 0.125
Outputs:
- layer_out: bfloat16 [32768, 2048], P(('sp', 'tp'))
The draws below stay inside these ranges and needn't reach their ends.
Inputs may be any that keep to these rules, and one draw needn't show every extreme that they name: `routes`: A token's 2 experts differ. In each aligned block of 128 tokens no expert is named by more than 8 tokens, a bound that some block reaches.
All inputs are finite; a program needn't handle non-finite values.
Results may differ from the reference program's by a relative error of at most 0.012.
Values may be sent and summed in bfloat16 or wider, within the bound.
A program may use at most 128 MiB of HBM per device.

```python
import math
import jax
import jax.numpy as jnp
import numpy as np
from jax import lax

D = 2048
FE = 2048
TOP = 2
TAPS = 3
TOK_DEV = 512
TOKQ = 128
EXPERTS = 64
CAPQ = 8
TOKENS = 32768
N_SP = 64
N_TP = 4


def levels(key, shape, shards, least, largest):
    gain, own = 1.0, jax.random.fold_in(key, 6)
    for position, blocks in shards:
        heights = jnp.exp(jax.random.uniform(jax.random.fold_in(own, position), (blocks,), jnp.float32, least / len(shards), largest / len(shards)))
        gain = gain * jnp.repeat(heights, shape[position] // blocks).reshape([-1 if axis == position else 1 for axis in range(len(shape))])
    return gain


def routed_block(key, own, number, rows, count, top, bound, lean):
    sequence = jax.random.permutation(key, count)
    heavy_load, ordinary = shares(count, rows * top, bound, lean, True), shares(count, rows * top, bound, lean, False)
    places = jnp.arange(count)

    def named(lengths, rotation):
        used = int((lengths > 0).sum())
        fixed = max(1, used // 4)
        moved = fixed + (places - fixed + rotation * (used - fixed)) % max(1, count - fixed)
        return jnp.zeros((count,), jnp.int32).at[sequence[jnp.where(places < fixed, places, moved)]].set(jnp.asarray(lengths, jnp.int32))

    lengths = jnp.where(number % 4 == 0, named(heavy_load, number // 4), named(ordinary, number - number // 4 - 1))
    mixed = jax.random.permutation(jax.random.fold_in(own, 3), count)
    giver, sink = mixed[0:count // 2 * 2:2], mixed[1:count // 2 * 2:2]
    slack = jnp.minimum(lengths[giver] - 1, bound - lengths[sink]) // 2
    slack = jnp.where((giver == sequence[0]) | (sink == sequence[0]) | (lengths[sink] == 0), 0, jnp.maximum(slack, 0))
    moved = jax.random.randint(jax.random.fold_in(own, 4), (count // 2,), 0, 1 << 20) % (slack + 1)
    lengths = lengths.at[giver].add(-moved).at[sink].add(moved)
    items = jnp.searchsorted(jnp.cumsum(lengths), jnp.arange(rows * top), side="right").astype(jnp.int32)
    table = items.reshape(top, rows).T
    table = table[jax.random.permutation(jax.random.fold_in(own, 1), rows)]
    rotation = jax.random.randint(jax.random.fold_in(own, 2), (rows, 1), 0, top)
    return jnp.take_along_axis(table, (jnp.arange(top)[None, :] + rotation) % top, axis=1)


def shares(count, total, most, slope, full):
    loads = [(1 << 20) // math.isqrt(rank ** slope) + 1 for rank in range(1, count + 1)]
    largest = most if full else min(most, max(-(-total // count), total * loads[0] // sum(loads)))
    least = 1 if total - largest >= count - 1 else 0
    given, rest = [largest] + [least] * (count - 1), total - largest - least * (count - 1)
    while rest > 0:
        candidates = [i for i in range(1, count) if given[i] < largest] or [i for i in range(1, count) if given[i] < most]
        pool, left = sum([loads[i] for i in candidates]), rest
        for i in candidates:
            extra = min(most - given[i], max(1, left * loads[i] // pool), rest)
            given[i] = given[i] + extra
            rest = rest - extra
    return np.array(given)


def bell_draw(key, extent, spread, reach, cuts=(), kind=jnp.bfloat16):
    array = jax.random.normal(key, extent, jnp.float32) * spread
    if len(cuts) > 0:
        array = levels(key, extent, cuts, -0.22, 0.18) * array
    return jnp.clip(array, min=-reach, max=reach).astype(kind)


def setup_inputs(seed: int = 0) -> dict:
    key_list = jax.random.split(jax.random.key(seed), 13)
    gate_in = bell_draw(key_list[0], (TOKENS, D), 1.0, 6.0, ((0, 64), (1, 4)))
    value_in = bell_draw(key_list[1], (TOKENS, D), 1.0, 6.0, ((0, 64), (1, 4)))
    gate_out = bell_draw(key_list[2], (TOKENS, D), 1.0, 6.0, ((0, 64), (1, 4)))
    conv_taps = bell_draw(key_list[3], (TAPS, D), TAPS ** -0.5, 3.5, ((1, 4),), jnp.float32)
    proj_weight = bell_draw(key_list[4], (D, D), D ** -0.5, 0.125, ((0, 4),))
    residual = bell_draw(key_list[5], (TOKENS, D), 1.0, 6.0, ((0, 256),))
    norm_gain = jnp.clip(1.0 + 0.18 * jax.random.normal(key_list[6], (D,), jnp.float32), 0.1, 1.9)
    routes_keys = jax.random.split(jax.random.fold_in(key_list[7], 1), TOKENS // TOKQ)
    routes_turns = jax.random.permutation(jax.random.fold_in(key_list[7], 3), TOKENS // TOKQ)
    routes = jax.vmap(lambda own, number: routed_block(jax.random.fold_in(key_list[7], 2), own, number, TOKQ, EXPERTS, TOP, CAPQ, 2))(routes_keys, routes_turns).reshape((TOKENS, TOP))
    route_weight = jnp.clip(0.1 + 0.79999997 * jax.random.uniform(key_list[8], (TOKENS, TOP), jnp.float32) ** levels(key_list[8], (TOKENS, TOP), ((0, 64),), -0.2, 0.2), 0.1, 0.9)
    expert_gate = bell_draw(key_list[9], (EXPERTS, D, FE), D ** -0.5, 0.125, ((0, 64), (2, 4)))
    expert_up = bell_draw(key_list[10], (EXPERTS, D, FE), D ** -0.5, 0.125, ((0, 64), (2, 4)))
    expert_down = bell_draw(key_list[11], (EXPERTS, FE, D), FE ** -0.5, 0.125, ((0, 64), (1, 4)))
    return dict(gate_in=gate_in, value_in=value_in, gate_out=gate_out, conv_taps=conv_taps, proj_weight=proj_weight, residual=residual, norm_gain=norm_gain, routes=routes, route_weight=route_weight, expert_gate=expert_gate, expert_up=expert_up, expert_down=expert_down)


def rounded(values):
    return lax.optimization_barrier(values.astype(jnp.bfloat16)).astype(jnp.float32)

def slot_numbers(route_ids, block_rows, expert_count):
    block_count = route_ids.shape[0] // block_rows
    flat_ids = route_ids.reshape(block_count, block_rows * route_ids.shape[1])
    one_hot = (flat_ids[:, :, None] == jnp.arange(expert_count, dtype=jnp.int32)[None, None, :]).astype(jnp.int32)
    before = jnp.cumsum(one_hot, axis=1) - one_hot
    return lax.optimization_barrier(jnp.sum(before * one_hot, axis=2)).reshape(route_ids.shape).astype(jnp.int32)

def normalize(hidden_rows, norm_gain):
    inverse = lax.rsqrt(lax.optimization_barrier(jnp.mean(hidden_rows * hidden_rows, axis=-1, keepdims=True)) + 1e-05)
    return (hidden_rows * inverse * norm_gain.astype(jnp.float32)).astype(jnp.bfloat16)

def mixer_output(gate_in, value_in, gate_out, conv_taps, prior_gate, prior_value):
    product = gate_in.astype(jnp.float32) * value_in.astype(jnp.float32)
    prior_mix = prior_gate.astype(jnp.float32) * prior_value.astype(jnp.float32)
    padded = jnp.concatenate([prior_mix, product], axis=0)
    taps = conv_taps.astype(jnp.float32)
    conv_sum = taps[0] * padded[:-2] + taps[1] * padded[1:-1] + taps[2] * padded[2:]
    return (gate_out.astype(jnp.float32) * conv_sum).astype(jnp.bfloat16)

def reference(gate_in, value_in, gate_out, conv_taps, proj_weight, residual, norm_gain, routes, route_weight, expert_gate, expert_up, expert_down):
    model_width = residual.shape[1]
    zero_rows = jnp.zeros((2, gate_in.shape[1]), jnp.bfloat16)
    mixed_out = mixer_output(gate_in, value_in, gate_out, conv_taps, zero_rows, zero_rows)
    slice_width = model_width // N_TP
    summed = jnp.zeros(residual.shape, jnp.float32)
    for group in range(N_TP):
        lower = group * slice_width
        summed = summed + rounded(jnp.dot(mixed_out[:, lower:lower + slice_width], proj_weight[lower:lower + slice_width], preferred_element_type=jnp.float32))
    hidden_rows = residual.astype(jnp.float32) + summed
    normed = normalize(hidden_rows, norm_gain)
    token_count = residual.shape[0]
    top_count = routes.shape[1]
    slots = slot_numbers(routes, TOKQ, EXPERTS)
    token_ids = jnp.arange(token_count, dtype=jnp.int32)
    source = token_ids // TOK_DEV
    quarter = token_ids % TOK_DEV // TOKQ
    flat_index = ((routes * N_TP + quarter[:, None]) * N_SP + source[:, None]) * CAPQ + slots
    per_expert = N_TP * N_SP * CAPQ
    slot_count = EXPERTS * per_expert
    slot_token = jnp.full((slot_count,), token_count, jnp.int32).at[flat_index.reshape(-1)].set(jnp.repeat(token_ids, top_count))
    slot_weight = jnp.zeros((slot_count,), jnp.float32).at[flat_index.reshape(-1)].set(route_weight.reshape(-1))
    padded_rows = jnp.concatenate([normed, jnp.zeros((1, model_width), jnp.bfloat16)], axis=0)
    hidden_width = expert_gate.shape[2] // N_TP

    def one_expert(total, expert):
        start_row = (expert * per_expert).astype(jnp.int32)
        chosen = lax.dynamic_slice_in_dim(slot_token, start_row, per_expert, 0)
        weights_now = lax.dynamic_slice_in_dim(slot_weight, start_row, per_expert, 0)
        row_block = padded_rows[chosen]
        gate_pre = jnp.dot(row_block, expert_gate[expert], preferred_element_type=jnp.float32)
        up_pre = jnp.dot(row_block, expert_up[expert], preferred_element_type=jnp.float32)
        hidden = (jax.nn.silu(gate_pre) * up_pre).astype(jnp.bfloat16)
        down_weight = expert_down[expert]
        partial_sum = jnp.zeros((per_expert, model_width), jnp.float32)
        for group in range(N_TP):
            lower = group * hidden_width
            partial_sum = partial_sum + rounded(jnp.dot(hidden[:, lower:lower + hidden_width], down_weight[lower:lower + hidden_width], preferred_element_type=jnp.float32))
        expert_rows = rounded(partial_sum)
        total = total.at[chosen].add(weights_now[:, None] * expert_rows)
        return (total, None)
    total, _ = lax.scan(one_expert, jnp.zeros((token_count + 1, model_width), jnp.float32), jnp.arange(EXPERTS, dtype=jnp.int32))
    return (hidden_rows + total[:token_count]).astype(jnp.bfloat16)
```

```python
import jax
import jax.numpy as jnp
from jax import lax
from jax.sharding import PartitionSpec as P


def swapped(shard, first):
    sp_count, tp_count = lax.axis_size("sp"), lax.axis_size("tp")
    pairs = []
    for s in range(sp_count):
        for t in range(tp_count):
            other = t ^ 1 if (s % 2 == 0) == first else tp_count - 1 - t
            pairs.append((s * tp_count + t, s * tp_count + other))
    return lax.ppermute(shard, ("sp", "tp"), pairs)


def passed_along(shard, axis, by):
    size = lax.axis_size(axis)
    pairs = [(i, i + by) for i in range(size) if 0 <= i + by < size]
    return lax.ppermute(shard, axis, pairs)


def split_up(shard, dim, size):
    before, after = (shard.shape[:dim], shard.shape[dim + 1 :])
    return jnp.moveaxis(shard.reshape(*before, size, -1, *after), dim, 0)


def sum_at_owner(shard, axis, dim):
    parts = split_up(shard, dim, lax.axis_size(axis))
    arrived = lax.all_to_all(parts, axis, split_axis=0, concat_axis=0, tiled=True)
    return arrived.astype(jnp.float32).sum(axis=0)


def rounded(values):
    return lax.optimization_barrier(values.astype(jnp.bfloat16)).astype(jnp.float32)


def slot_numbers(route_ids, block_rows, expert_count):
    block_count = route_ids.shape[0] // block_rows
    flat_ids = route_ids.reshape(block_count, block_rows * route_ids.shape[1])
    one_hot = (
        flat_ids[:, :, None] == jnp.arange(expert_count, dtype=jnp.int32)[None, None, :]
    ).astype(jnp.int32)
    before = jnp.cumsum(one_hot, axis=1) - one_hot
    return jnp.sum(before * one_hot, axis=2).reshape(route_ids.shape)


def normalize(hidden_rows, norm_gain):
    inverse = lax.rsqrt(jnp.mean(hidden_rows * hidden_rows, axis=-1, keepdims=True) + 1e-05)
    return (hidden_rows * inverse * norm_gain).astype(jnp.bfloat16)


def dispatch_rows(normed, route_ids, block_rows, expert_count, capacity):
    row_count = route_ids.shape[0]
    top_count = route_ids.shape[1]
    block_count = row_count // block_rows
    slots = slot_numbers(route_ids, block_rows, expert_count)
    row_ids = jnp.arange(row_count, dtype=jnp.int32)
    flat_index = ((row_ids // block_rows)[:, None] * expert_count + route_ids) * capacity + slots
    slot_token = (
        jnp.full((block_count * expert_count * capacity,), row_count, jnp.int32)
        .at[flat_index.reshape(-1)]
        .set(jnp.repeat(row_ids, top_count))
    )
    padded_rows = jnp.concatenate([normed, jnp.zeros((1, normed.shape[1]), jnp.bfloat16)], axis=0)
    outgoing = padded_rows[slot_token].reshape(block_count, expert_count, capacity, normed.shape[1])
    return (outgoing, slots)


def body(
    gate_in,
    value_in,
    gate_out,
    conv_taps,
    proj_weight,
    residual,
    norm_gain,
    routes,
    route_weight,
    expert_gate,
    expert_up,
    expert_down,
):
    tok_dev = gate_in.shape[0]
    model_width = residual.shape[1]
    tp_count = lax.axis_size("tp")
    groups = lax.axis_size("sp")
    quarter = residual.shape[0]
    top_count = routes.shape[1]
    capacity = 2 * quarter * top_count // groups
    tp_index = lax.axis_index("tp")
    first_own = tp_index * quarter
    gates = (expert_gate[0], swapped(expert_gate[0], True))
    ups = (expert_up[0], swapped(expert_up[0], True))
    downs = (expert_down[0], swapped(expert_down[0], True))
    prior_gate, prior_value = passed_along(
        (gate_in[tok_dev - 2 :], value_in[tok_dev - 2 :]), "sp", 1
    )
    product = gate_in.astype(jnp.float32) * value_in.astype(jnp.float32)
    prior_mix = prior_gate.astype(jnp.float32) * prior_value.astype(jnp.float32)
    padded = jnp.concatenate([prior_mix, product], axis=0)
    conv_sum = conv_taps[0] * padded[:-2] + conv_taps[1] * padded[1:-1] + conv_taps[2] * padded[2:]
    mixed_out = (gate_out.astype(jnp.float32) * conv_sum).astype(jnp.bfloat16)
    own_routes = lax.dynamic_slice_in_dim(routes, first_own, quarter, 0)
    own_weights = lax.dynamic_slice_in_dim(route_weight, first_own, quarter, 0)
    summed = sum_at_owner(
        rounded(jnp.dot(mixed_out, proj_weight, preferred_element_type=jnp.float32)).astype(
            jnp.bfloat16
        ),
        "tp",
        0,
    )
    my_rows = residual.astype(jnp.float32) + summed
    normed = normalize(my_rows, norm_gain)
    outgoing, own_slots = dispatch_rows(normed, own_routes, quarter, groups, capacity)
    own_arrived = lax.all_to_all(outgoing, "sp", split_axis=1, concat_axis=1, tiled=True)
    own_flat = own_arrived.reshape(groups * capacity, model_width)
    other_flat = swapped(own_flat, False)

    def hidden_of(rows):
        hidden = []
        for gate, up in zip(gates, ups):
            gate_pre = jnp.dot(rows, gate, preferred_element_type=jnp.float32)
            up_pre = jnp.dot(rows, up, preferred_element_type=jnp.float32)
            hidden.append((jax.nn.silu(gate_pre) * up_pre).astype(jnp.bfloat16))
        return hidden

    def down_of(hidden):
        total = jnp.dot(hidden[0], downs[0], preferred_element_type=jnp.float32)
        return total + jnp.dot(hidden[1], downs[1], preferred_element_type=jnp.float32)

    own_hidden = hidden_of(own_flat)
    other_partial = down_of(hidden_of(other_flat)).astype(jnp.bfloat16)
    arrived_partial = swapped(other_partial, False)
    expert_rows = (down_of(own_hidden) + arrived_partial.astype(jnp.float32)).astype(jnp.bfloat16)
    returned = lax.all_to_all(
        expert_rows.reshape(groups, capacity, model_width),
        "sp",
        split_axis=0,
        concat_axis=0,
        tiled=True,
    )
    flat_pick = own_routes * capacity + own_slots
    picked = returned.reshape(groups * capacity, model_width)[flat_pick]
    weighted = jnp.sum(own_weights[:, :, None] * picked.astype(jnp.float32), axis=1)
    return (my_rows + weighted).astype(jnp.bfloat16)


def solution(mesh):
    placed = (
        P("sp", "tp"),
        P("sp", "tp"),
        P("sp", "tp"),
        P(None, "tp"),
        P("tp", None),
        P(("sp", "tp"), None),
        P(),
        P("sp", None),
        P("sp", None),
        P("sp", None, "tp"),
        P("sp", None, "tp"),
        P("sp", "tp", None),
    )
    return jax.shard_map(
        body, mesh=mesh, in_specs=placed, out_specs=P(("sp", "tp"), None), check_vma=False
    )
```
